32 devices in a mesh: sp: 8 (over z, x), tp: 4 (over y, core).
Axes of the slice: x: 2, y: 2, z: 4, core: 2. Of those that a mesh axis runs over, the one named last changes fastest.
Arguments:
- query_one: bfloat16 [2048, 1024], P('sp', 'tp'), may hold values from -6 to 6
- key_one: bfloat16 [2048, 1024], P('sp', 'tp'), may hold values from -6 to 6
- value_one: bfloat16 [2048, 2048], P('sp', 'tp'), may hold values from -6 to 6
- gate_one: bfloat16 [2048, 2048], P('sp', 'tp'), may hold values from -6 to 6
- decay_one: float32 [2, 2048, 1024], P(None, 'sp', 'tp')
- query_two: bfloat16 [2048, 2048], P('sp', 'tp'), may hold values from -6 to 6
- key_two: bfloat16 [2048, 2048], P('sp', 'tp'), may hold values from -6 to 6
- value_two: bfloat16 [2048, 2048], P('sp', 'tp'), may hold values from -6 to 6
- gate_two: bfloat16 [2048, 2048], P('sp', 'tp'), may hold values from -6 to 6
- decay_two: float32 [2, 2048, 2048], P(None, 'sp', 'tp')
- head_gain: float32 [128], replicated, may hold values from 0.1 to 1.9
- proj_one: bfloat16 [2048, 2048], P('tp'), may hold values from -0.09375 to 0.09375
- proj_two: bfloat16 [2048, 2048], P('tp'), may hold values from -0.09375 to 0.09375
- stream: bfloat16 [2048, 2048], P('sp'), may hold values from -6 to 6
- gain_mix: float32 [2048], replicated, may hold values from 0.1 to 1.9
- gain_moe: float32 [2048], replicated, may hold values from 0.1 to 1.9
- routes: int32 [2048, 2], P('sp'), may hold values from 0 to 7, all different within a row; in each aligned block of 256 rows (0 to 255, 256 to 511, ...) at most 96 rows name the same one
- affinity: float32 [2048, 2], P('sp'), may hold values from 0.1 to 1
- expert_gate: bfloat16 [8, 2048, 2048], P('sp', None, 'tp'), may hold values from -0.125 to 0.125
- expert_up: bfloat16 [8, 2048, 2048], P('sp', None, 'tp'), may hold values from -0.125 to 0.125
- expert_down: bfloat16 [8, 2048, 2048], P('sp', 'tp'), may hold values from -0.125 to 0.125
Outputs:
- output: bfloat16 [2048, 2048], P(('sp', 'tp'))
The draws below stay inside these ranges and needn't reach their ends.
Inputs may be any that keep to these rules, and one draw needn't show every extreme that they name: `routes`: in the 256 rows of one index of sp no expert is named more than 96 times, a bound that some block reaches there in every draw; a row names 2 different experts.
All inputs are finite; a program needn't handle non-finite values.
Results may differ from the reference program's by a relative error of at most 0.017.
Values may be sent and summed in bfloat16 or wider, within the bound.
A program may use at most 64 MiB of HBM per device.

```python
import math
import jax
import jax.numpy as jnp
import numpy as np
from jax import lax

D = 2048
HEADS_A = 16
HEADS_B = 16
DK_A = 64
DK_B = 128
DV = 128
BLK = 64
FF_E = 2048
TOPK = 2
TOK_DEV = 256
STRING_LENGTH = 2048
EXPERTS = 8
CAP = 96
N_SP = 8
N_TP = 4


def decay_field(key, channels):
    keys = jax.random.split(key, 7)
    share = 0.5
    rapid_toggle = jax.random.bernoulli(keys[0], share, (2, 1, channels))
    quick = jax.random.uniform(keys[1], (2, 1, channels), jnp.float32, -0.5, 1.5)
    steady = math.log(STRING_LENGTH / 16.0) + jax.random.uniform(keys[2], (2, 1, channels), jnp.float32, 0.5, 1.5)
    floor_amount = jnp.where(rapid_toggle, quick, steady)
    spans = STRING_LENGTH // TOK_DEV
    additive_displacement = jnp.repeat(jax.random.uniform(keys[3], (2, spans, 1), jnp.float32, -0.7, 0.7), TOK_DEV, axis=1)
    jitter_magnitude = 0.7 * jax.random.truncated_normal(keys[4], -3.0, 3.0, (2, STRING_LENGTH, channels), jnp.float32)
    slot_numbers = jax.random.randint(keys[5], (2, 6), 0, STRING_LENGTH)
    sudden_jump = jnp.any(jnp.arange(STRING_LENGTH)[None, :, None] == slot_numbers[:, None, :], axis=2)[:, :, None]
    intensity_multiplier = jax.random.uniform(keys[6], (2, STRING_LENGTH, 1), jnp.float32, -11.0, -4.0)
    return jnp.where(sudden_jump & jnp.logical_not(rapid_toggle), intensity_multiplier, floor_amount + additive_displacement + jitter_magnitude).astype(jnp.float32)


def draw_decay_one(key, part):
    return decay_field(jax.random.fold_in(key, 11), HEADS_A * DK_A)


def draw_decay_two(key, part):
    return decay_field(jax.random.fold_in(key, 23), HEADS_B * DK_B)


def shard_levels(rng, shape, shards, smallest, high):
    level = 1.0
    for axis_at, shards_of in shards:
        heights = jax.random.uniform(jax.random.fold_in(jax.random.fold_in(rng, 6), axis_at), (shards_of,), jnp.float32, smallest / len(shards), high / len(shards))
        level = level * jnp.repeat(jnp.exp(heights), shape[axis_at] // shards_of).reshape((-1,) + (1,) * (len(shape) - 1 - axis_at))
    return level


def routed_block(stream_key, own, number, rows, count, top, bound, slope):
    ranking = jax.random.permutation(stream_key, count)
    packed, common = shares(count, rows * top, bound, slope, True), shares(count, rows * top, bound, slope, False)
    places = jnp.arange(count)

    def named(tallies, turn):
        used = int((tallies > 0).sum())
        fixed = max(1, used // 4)
        moved = fixed + (places - fixed + turn * (used - fixed)) % max(1, count - fixed)
        return jnp.zeros((count,), jnp.int32).at[ranking[jnp.where(places < fixed, places, moved)]].set(jnp.asarray(tallies, jnp.int32))

    tallies = jnp.where(number % 4 == 0, named(packed, number // 4), named(common, number - number // 4 - 1))
    mixed = jax.random.permutation(jax.random.fold_in(own, 3), count)
    donor, receiver = mixed[0:count // 2 * 2:2], mixed[1:count // 2 * 2:2]
    margin = jnp.minimum(tallies[donor] - 1, bound - tallies[receiver]) // 2
    margin = jnp.where((donor == ranking[0]) | (receiver == ranking[0]) | (tallies[receiver] == 0), 0, jnp.maximum(margin, 0))
    moved = jax.random.randint(jax.random.fold_in(own, 4), (count // 2,), 0, 1 << 20) % (margin + 1)
    tallies = tallies.at[donor].add(-moved).at[receiver].add(moved)
    labels = jnp.searchsorted(jnp.cumsum(tallies), jnp.arange(rows * top), side="right").astype(jnp.int32)
    listing = labels.reshape(top, rows).T
    listing = listing[jax.random.permutation(jax.random.fold_in(own, 1), rows)]
    turn = jax.random.randint(jax.random.fold_in(own, 2), (rows, 1), 0, top)
    return jnp.take_along_axis(listing, (jnp.arange(top)[None, :] + turn) % top, axis=1)


def shares(amount, total, bound, slope, full):
    loads = [(1 << 20) // math.isqrt(rank ** slope) + 1 for rank in range(1, amount + 1)]
    largest = bound if full else min(bound, max(-(-total // amount), total * loads[0] // sum(loads)))
    least = 1 if total - largest >= amount - 1 else 0
    given, rest = [largest] + [least] * (amount - 1), total - largest - least * (amount - 1)
    while rest > 0:
        movable = [i for i in range(1, amount) if given[i] < largest] or [i for i in range(1, amount) if given[i] < bound]
        pool, left = sum([loads[i] for i in movable]), rest
        for i in movable:
            addition = min(bound - given[i], max(1, left * loads[i] // pool), rest)
            given[i] = given[i] + addition
            rest = rest - addition
    return np.array(given)


def centred(own_key, extent, scale, limit, pieces=(), kind=jnp.bfloat16):
    values = jax.random.normal(own_key, extent, jnp.float32) * scale
    if len(pieces) > 0:
        values = shard_levels(own_key, extent, pieces, -0.22, 0.18) * values
    return jnp.clip(values, min=-limit, max=limit).astype(kind)


def setup_inputs(seed: int = 0) -> dict:
    seeds = jax.random.split(jax.random.key(seed), 22)
    query_one = centred(seeds[0], (STRING_LENGTH, HEADS_A * DK_A), 1.0, 6.0, ((0, 8), (1, 4)))
    key_one = centred(seeds[1], (STRING_LENGTH, HEADS_A * DK_A), 1.0, 6.0, ((0, 8), (1, 4)))
    value_one = centred(seeds[2], (STRING_LENGTH, HEADS_A * DV), 1.0, 6.0, ((0, 8), (1, 4)))
    gate_one = centred(seeds[3], (STRING_LENGTH, HEADS_A * DV), 1.0, 6.0, ((0, 8), (1, 4)))
    decay_one = draw_decay_one(jax.random.fold_in(seeds[21], 71), 0)
    query_two = centred(seeds[5], (STRING_LENGTH, HEADS_B * DK_B), 1.0, 6.0, ((0, 8), (1, 4)))
    key_two = centred(seeds[6], (STRING_LENGTH, HEADS_B * DK_B), 1.0, 6.0, ((0, 8), (1, 4)))
    value_two = centred(seeds[7], (STRING_LENGTH, HEADS_B * DV), 1.0, 6.0, ((0, 8), (1, 4)))
    gate_two = centred(seeds[8], (STRING_LENGTH, HEADS_B * DV), 1.0, 6.0, ((0, 8), (1, 4)))
    decay_two = draw_decay_two(jax.random.fold_in(seeds[21], 71), 0)
    head_gain = jnp.clip(1.0 + 0.18 * jax.random.normal(seeds[10], (DV,), jnp.float32), 0.1, 1.9)
    proj_one = centred(seeds[11], (HEADS_A * DV, D), ((HEADS_A + HEADS_B) * DV) ** -0.5, 0.09375, ((0, 4),))
    proj_two = centred(seeds[12], (HEADS_B * DV, D), ((HEADS_A + HEADS_B) * DV) ** -0.5, 0.09375, ((0, 4),))
    stream = centred(seeds[13], (STRING_LENGTH, D), 1.0, 6.0, ((0, 8),))
    gain_mix = jnp.clip(1.0 + 0.18 * jax.random.normal(seeds[14], (D,), jnp.float32), 0.1, 1.9)
    gain_moe = jnp.clip(1.0 + 0.18 * jax.random.normal(seeds[15], (D,), jnp.float32), 0.1, 1.9)
    routes_keys = jax.random.split(jax.random.fold_in(seeds[16], 1), STRING_LENGTH // TOK_DEV)
    routes_turns = jax.random.permutation(jax.random.fold_in(seeds[16], 3), STRING_LENGTH // TOK_DEV)
    routes = jax.vmap(lambda own, number: routed_block(jax.random.fold_in(seeds[16], 2), own, number, TOK_DEV, EXPERTS, TOPK, CAP, 2))(routes_keys, routes_turns).reshape((STRING_LENGTH, TOPK))
    affinity = jnp.clip(0.1 + 0.9 * jax.random.uniform(seeds[17], (STRING_LENGTH, TOPK), jnp.float32) ** shard_levels(seeds[17], (STRING_LENGTH, TOPK), ((0, 8),), -0.2, 0.2), 0.1, 1.0)
    expert_gate = centred(seeds[18], (EXPERTS, D, FF_E), D ** -0.5, 0.125, ((0, 8), (2, 4)))
    expert_up = centred(seeds[19], (EXPERTS, D, FF_E), D ** -0.5, 0.125, ((0, 8), (2, 4)))
    expert_down = centred(seeds[20], (EXPERTS, FF_E, D), FF_E ** -0.5, 0.125, ((0, 8), (1, 4)))
    return {"query_one": query_one, "key_one": key_one, "value_one": value_one, "gate_one": gate_one, "decay_one": decay_one, "query_two": query_two, "key_two": key_two, "value_two": value_two, "gate_two": gate_two, "decay_two": decay_two, "head_gain": head_gain, "proj_one": proj_one, "proj_two": proj_two, "stream": stream, "gain_mix": gain_mix, "gain_moe": gain_moe, "routes": routes, "affinity": affinity, "expert_gate": expert_gate, "expert_up": expert_up, "expert_down": expert_down}


normalizer_sharpness = 16.0
highest = lax.Precision.HIGHEST

def heads_first(values, heads):
    return values.reshape(values.shape[0], heads, -1).transpose(1, 0, 2)

def block_scan(query, key, value, logarithm_fading):
    heads, length, key_size = query.shape
    value_size = value.shape[-1]
    count = length // BLK

    def blocks(tensor):
        return tensor.reshape(heads, count, BLK, tensor.shape[-1])
    qb, kb, vb, gb = (blocks(query), blocks(key), blocks(value), blocks(logarithm_fading))
    cum = jnp.cumsum(gb, axis=2)
    last = cum[:, :, -1:, :]
    q_in = qb * jnp.exp(cum)
    k_in = kb * jnp.exp(-cum)
    k_st = kb * jnp.exp(last - cum)
    lower = jnp.tril(jnp.ones((BLK, BLK), dtype=bool))
    scores = jnp.where(lower, jnp.einsum('hnid,hnjd->hnij', q_in, k_in, precision=highest), 0.0)
    inner = jnp.einsum('hnij,hnjv->hniv', scores, vb, precision=highest)
    growth = jnp.einsum('hnjd,hnjv->hndv', k_st, vb, precision=highest)
    fading_speed = jnp.exp(last[:, :, 0, :])

    def step(state, inputs):
        factor, added = inputs
        return (factor[..., None] * state + added, state)
    final, starts = lax.scan(step, jnp.zeros((heads, key_size, value_size), jnp.float32), (fading_speed.transpose(1, 0, 2), growth.transpose(1, 0, 2, 3)))
    carried = jnp.einsum('hnid,hndv->hniv', q_in, starts.transpose(1, 0, 2, 3), precision=highest)
    return ((inner + carried).reshape(heads, length, value_size), final)

def group_mixed(query, key, value, fading_speed, key_size):
    heads = query.shape[1] // key_size
    qh = heads_first(query.astype(jnp.float32), heads) * key_size ** (-0.5)
    kh = heads_first(key.astype(jnp.float32), heads)
    vh = heads_first(value.astype(jnp.float32), heads)
    logarithm_fading = jax.nn.log_sigmoid(fading_speed) / normalizer_sharpness
    ahead = heads_first(logarithm_fading[0], heads)
    behind = heads_first(logarithm_fading[1], heads)
    forward, _ = block_scan(qh, kh, vh, ahead)
    backward, _ = block_scan(qh[:, ::-1], kh[:, ::-1], vh[:, ::-1], behind[:, ::-1])
    return forward + backward[:, ::-1]

def finish(mixed, gate, head_gain):
    normed = mixed * lax.rsqrt(lax.optimization_barrier(jnp.mean(mixed * mixed, axis=-1, keepdims=True)) + 1e-06) * head_gain
    flat = normed.transpose(1, 0, 2).reshape(mixed.shape[1], -1)
    return (flat * jax.nn.silu(gate.astype(jnp.float32))).astype(jnp.bfloat16)

def layer_norm(values, gain):
    mean = lax.optimization_barrier(jnp.mean(values, axis=-1, keepdims=True))
    spread = lax.optimization_barrier(jnp.mean(jnp.square(values - mean), axis=-1, keepdims=True))
    return (values - mean) * lax.rsqrt(spread + 1e-05) * gain

def reference(query_one, key_one, value_one, gate_one, decay_one, query_two, key_two, value_two, gate_two, decay_two, head_gain, proj_one, proj_two, stream, gain_mix, gain_moe, routes, affinity, expert_gate, expert_up, expert_down):
    heads_one = finish(group_mixed(query_one, key_one, value_one, decay_one, DK_A), gate_one, head_gain)
    heads_two = finish(group_mixed(query_two, key_two, value_two, decay_two, DK_B), gate_two, head_gain)
    width_one = HEADS_A // N_TP * DV
    width_two = HEADS_B // N_TP * DV
    total = jnp.zeros((STRING_LENGTH, D), jnp.float32)
    for block in range(N_TP):
        part = jnp.dot(heads_one[:, block * width_one:(block + 1) * width_one], proj_one[block * width_one:(block + 1) * width_one], preferred_element_type=jnp.float32)
        part = part + jnp.dot(heads_two[:, block * width_two:(block + 1) * width_two], proj_two[block * width_two:(block + 1) * width_two], preferred_element_type=jnp.float32)
        total = total + lax.optimization_barrier(part.astype(jnp.bfloat16)).astype(jnp.float32)
    attn = total.astype(jnp.bfloat16)
    settled = layer_norm(stream.astype(jnp.float32) + attn.astype(jnp.float32), gain_mix)
    moe_in = settled.astype(jnp.bfloat16)
    weights = (affinity / lax.optimization_barrier(jnp.sum(affinity, axis=-1, keepdims=True))).reshape(-1)
    assigned = STRING_LENGTH * TOPK
    flat_expert = routes.reshape(-1).astype(jnp.int32)
    order = jnp.argsort(flat_expert, stable=True).astype(jnp.int32)
    sorted_expert = flat_expert[order]
    counts = lax.optimization_barrier(jnp.sum((flat_expert[:, None] == jnp.arange(EXPERTS, dtype=jnp.int32)[None, :]).astype(jnp.int32), axis=0)).astype(jnp.int32)
    starts = (jnp.cumsum(counts).astype(jnp.int32) - counts).astype(jnp.int32)
    most_rows = N_SP * CAP
    slot = (jnp.arange(assigned, dtype=jnp.int32) - starts[sorted_expert]).astype(jnp.int32)
    table = jnp.full((EXPERTS * most_rows,), -1, jnp.int32).at[sorted_expert * most_rows + slot].set(order)
    table = table.reshape(EXPERTS, most_rows)
    unit_block = FF_E // N_TP

    def per_expert(acc, expert):
        entries = table[expert]
        valid = entries >= 0
        safe = jnp.where(valid, entries, 0).astype(jnp.int32)
        token = (safe // TOPK).astype(jnp.int32)
        rows = moe_in[token]
        gate = jnp.dot(rows, expert_gate[expert], preferred_element_type=jnp.float32)
        upward = jnp.dot(rows, expert_up[expert], preferred_element_type=jnp.float32)
        act = (jax.nn.silu(gate) * upward).astype(jnp.bfloat16)
        act_blocks = act.astype(jnp.float32).reshape(most_rows, N_TP, unit_block)
        down_blocks = expert_down[expert].astype(jnp.float32).reshape(N_TP, unit_block, D)
        partial_value = jnp.einsum('rbf,bfd->rbd', act_blocks, down_blocks, precision=highest)
        rounded = lax.optimization_barrier(partial_value.astype(jnp.bfloat16)).astype(jnp.float32)
        piece = lax.optimization_barrier(lax.optimization_barrier(jnp.sum(rounded, axis=1)).astype(jnp.bfloat16)).astype(jnp.float32)
        scale = jnp.where(valid, weights[safe], 0.0)
        return (acc.at[token].add(scale[:, None] * piece), None)
    mixture, _ = lax.scan(per_expert, jnp.zeros((STRING_LENGTH, D), jnp.float32), jnp.arange(EXPERTS, dtype=jnp.int32))
    return layer_norm(settled + mixture, gain_moe).astype(jnp.bfloat16)
```

```python
import functools

import jax
import jax.numpy as jnp
from jax import lax
from jax.experimental import pallas as pl
from jax.experimental.pallas import tpu as pltpu
from jax.sharding import PartitionSpec as P

DK_A = 64
DK_B = 128
BLK = 64
SHARPNESS = 16.0
F32 = jnp.float32
BF16 = jnp.bfloat16
MESH = pl.DeviceIdType.MESH
VMEM = pl.BlockSpec(memory_space=pltpu.VMEM)
DMA = pltpu.SemaphoreType.DMA


def params(collective_id=None):
    if collective_id is None:
        return pltpu.CompilerParams(vmem_limit_bytes=48 * 2**20)
    return pltpu.CompilerParams(
        vmem_limit_bytes=48 * 2**20, collective_id=collective_id, has_side_effects=True
    )


def mm(a, b):
    return jnp.dot(a, b, preferred_element_type=F32)


def mm_nt(a, b):
    return lax.dot_general(a, b, (((1,), (1,)), ((), ())), preferred_element_type=F32)


def mm_tn(a, b):
    return lax.dot_general(a, b, (((0,), (0,)), ((), ())), preferred_element_type=F32)


def log_sigmoid(x):
    return jnp.minimum(x, 0.0) - jnp.log1p(jnp.exp(-jnp.abs(x)))


def silu(x):
    return x / (1.0 + jnp.exp(-x))


def layer_norm(values, gain):
    mean = jnp.mean(values, axis=-1, keepdims=True)
    spread = jnp.mean(jnp.square(values - mean), axis=-1, keepdims=True)
    return (values - mean) * lax.rsqrt(spread + 1e-05) * gain


def greet(peers):
    barrier = pltpu.get_barrier_semaphore()
    for peer in peers:
        pl.semaphore_signal(barrier, inc=1, device_id=peer, device_id_type=MESH)
    pl.semaphore_wait(barrier, len(peers))


def remote(src, dst, send, recv, peer):
    return pltpu.make_async_remote_copy(
        src_ref=src, dst_ref=dst, send_sem=send, recv_sem=recv, device_id=peer, device_id_type=MESH
    )


def across(me, k, n):
    place, bit = 0, 1
    while bit < n:
        digit = lax.rem(me // bit, 2)
        place = place + (1 - digit if k & bit else digit) * bit
        bit *= 2
    return place


def state_kernel(ka, va, da, kb, vb, db, stack, cum):
    rows = ka.shape[0]
    count = rows // BLK
    ii = lax.broadcasted_iota(jnp.int32, (rows, rows), 0)
    jj = lax.broadcasted_iota(jnp.int32, (rows, rows), 1)
    same = (ii // BLK) == (jj // BLK)
    lower = jnp.where(same & (ii >= jj), 1.0, 0.0).astype(BF16)
    upper = jnp.where(same & (ii <= jj), 1.0, 0.0).astype(BF16)
    base = 0
    for k, v, d, dk in ((ka, va, da, DK_A), (kb, vb, db, DK_B)):
        wide = k.shape[1]
        heads = wide // dk
        dv = v.shape[1] // heads
        keys = k[...].astype(F32)
        for way in range(2):
            fade = log_sigmoid(d[way]) / SHARPNESS
            high = fade.astype(BF16)
            low = (fade - high.astype(F32)).astype(BF16)
            tri = lower if way == 0 else upper
            total = mm(tri, high) + mm(tri, low)
            cum[way, :, base : base + wide] = total
            tail = jnp.zeros((1, wide), F32)
            weighted = [None] * count
            for b in reversed(range(count)) if way == 0 else range(count):
                part = total[b * BLK : (b + 1) * BLK]
                last = part[BLK - 1 : BLK] if way == 0 else part[0:1]
                weighted[b] = (keys[b * BLK : (b + 1) * BLK] * jnp.exp(last - part + tail)).astype(BF16)
                tail = tail + last
            weighted = jnp.concatenate(weighted, axis=0)
            states = [
                mm_tn(v[:, h * dv : (h + 1) * dv], weighted[:, h * dk : (h + 1) * dk]).astype(BF16)
                for h in range(heads)
            ]
            states = states[0] if heads == 1 else jnp.concatenate(states, axis=1)
            thigh = tail.astype(BF16).astype(F32)
            row = lax.broadcasted_iota(jnp.int32, (16, wide), 0)
            fades = jnp.where(row == 0, thigh, jnp.where(row == 1, tail - thigh, 0.0)).astype(BF16)
            half = dv // 2
            for i in range(2):
                stack[i, way, 0:half, base : base + wide] = states[i * half : (i + 1) * half]
                stack[i, way, half : half + 16, base : base + wide] = fades
        base += wide


def spread(total, wide):
    row = lax.broadcasted_iota(jnp.int32, (16, wide), 0)
    high = total.astype(BF16).astype(F32)
    return jnp.where(row == 0, high, jnp.where(row == 1, total - high, 0.0)).astype(BF16)


def states_exchange_kernel(n, stack, out, xbox, agg, zbox, outbox, xs, xr, zs, zr, bs, br):
    me = lax.axis_index("sp")
    side = lax.rem(me, 2)
    pair = me // 2
    pairs = n // 2
    partner = me + 1 - 2 * side
    half = out.shape[2]
    lanes = out.shape[3]
    chunk = 256 if lanes % 256 == 0 else lanes
    count = lanes // chunk

    def pair_at(j):
        return lax.rem(pair + j, pairs)

    greet([{"sp": partner}] + [{"sp": pair_at(j) * 2 + side} for j in range(1, pairs)])

    def at(c):
        return pl.ds(c * chunk, chunk)

    def swap(c):
        return remote(
            stack.at[1 - side, :, :, at(c)], xbox.at[:, :, at(c)], xs.at[c], xr.at[c], {"sp": partner}
        )

    def along(c, j):
        way = jnp.where(pair_at(j) < pair, 1, 0)
        return remote(
            agg.at[way, :, at(c)], zbox.at[pair, :, at(c)], zs.at[c, j], zr.at[c, j],
            {"sp": pair_at(j) * 2 + side},
        )

    def back(c):
        return remote(
            outbox.at[:, :, at(c)], out.at[:, side, :, at(c)], bs.at[c], br.at[c], {"sp": partner}
        )

    for c in range(count):
        swap(c).start()
    zbox[pair] = jnp.zeros_like(zbox[pair])

    def load(ref, index, c):
        block = ref[index + (slice(None), at(c))].astype(F32)
        return block[0:half], block[half : half + 1] + block[half + 1 : half + 2]

    def both(c, way):
        own, own_fade = load(stack, (side, way), c)
        other, other_fade = load(xbox, (way,), c)
        low = side == 0
        return (
            jnp.where(low, own, other), jnp.where(low, own_fade, other_fade),
            jnp.where(low, other, own), jnp.where(low, other_fade, own_fade),
        )

    for c in range(count):
        swap(c).wait_recv()
        s0, t0, s1, t1 = both(c, 0)
        agg[0, 0:half, at(c)] = (jnp.exp(t1) * s0 + s1).astype(BF16)
        agg[0, half : half + 16, at(c)] = spread(t0 + t1, chunk)
        s0, t0, s1, t1 = both(c, 1)
        agg[1, 0:half, at(c)] = (jnp.exp(t0) * s1 + s0).astype(BF16)
        agg[1, half : half + 16, at(c)] = spread(t0 + t1, chunk)
        for j in range(1, pairs):
            along(c, j).start()
    for c in range(count):
        for j in range(1, pairs):
            along(c, j).wait_recv()
        ahead = jnp.zeros((half, chunk), F32)
        behind = jnp.zeros((half, chunk), F32)
        for s in range(pairs):
            state, fade = load(zbox, (s,), c)
            ahead = jnp.where(s < pair, jnp.exp(fade) * ahead + state, ahead)
        for s in reversed(range(pairs)):
            state, fade = load(zbox, (s,), c)
            behind = jnp.where(s > pair, jnp.exp(fade) * behind + state, behind)
        low = side == 0
        s0, t0, _, _ = both(c, 0)
        next_ahead = jnp.exp(t0) * ahead + s0
        _, _, s1, t1 = both(c, 1)
        next_behind = jnp.exp(t1) * behind + s1
        outbox[0, :, at(c)] = jnp.where(low, next_ahead, ahead).astype(BF16)
        outbox[1, :, at(c)] = jnp.where(low, behind, next_behind).astype(BF16)
        back(c).start()
        out[0, side, :, at(c)] = jnp.where(low, ahead, next_ahead).astype(BF16)
        out[1, side, :, at(c)] = jnp.where(low, next_behind, behind).astype(BF16)
    for c in range(count):
        swap(c).wait_send()
        for j in range(1, pairs):
            along(c, j).wait_send()
        back(c).wait_send()
        remote(
            outbox.at[:, :, at(c)], out.at[:, 1 - side, :, at(c)], bs.at[c], br.at[c], {"sp": partner}
        ).wait_recv()


def mix_kernel(states, cum, qa, ka, va, ga, qb, kb, vb, gb, gain, pa, pb, out, heads_ref):
    rows = qa.shape[0]
    count = rows // BLK
    dv = gain.shape[1]
    ii = lax.broadcasted_iota(jnp.int32, (BLK, BLK), 0)
    jj = lax.broadcasted_iota(jnp.int32, (BLK, BLK), 1)
    base = 0
    column = 0
    for q, k, v, g, dk in ((qa, ka, va, ga, DK_A), (qb, kb, vb, gb, DK_B)):
        heads = q.shape[1] // dk
        for h in range(heads):
            lanes = slice(base + h * dk, base + (h + 1) * dk)
            own = slice(h * dk, (h + 1) * dk)
            vown = slice(h * dv, (h + 1) * dv)
            forward = jnp.concatenate([states[0, i, :, lanes] for i in range(2)], axis=0).astype(F32)
            backward = jnp.concatenate([states[1, i, :, lanes] for i in range(2)], axis=0).astype(F32)
            mixed = [None] * count
            readers = [None] * count
            growth = [None] * count
            for b in range(count):
                at = slice(b * BLK, (b + 1) * BLK)
                query = q[at, own].astype(F32) * dk ** (-0.5)
                key = k[at, own].astype(F32)
                value = v[at, vown]
                cf = cum[0, at, lanes]
                cb = cum[1, at, lanes]
                qf = (query * jnp.exp(cf)).astype(BF16)
                kf = (key * jnp.exp(-cf)).astype(BF16)
                qr = (query * jnp.exp(cb)).astype(BF16)
                kr = (key * jnp.exp(-cb)).astype(BF16)
                scores = jnp.where(ii >= jj, mm_nt(qf, kf), 0.0) + jnp.where(ii <= jj, mm_nt(qr, kr), 0.0)
                inner = mm(scores.astype(BF16), value)
                lastf = cf[BLK - 1 : BLK]
                inner = inner + mm_nt(qf, forward.astype(BF16))
                if b < count - 1:
                    kfs = (key * jnp.exp(lastf - cf)).astype(BF16)
                    forward = jnp.exp(lastf) * forward + mm_tn(value, kfs)
                mixed[b] = inner
                readers[b] = qr
                lastb = cb[0:1]
                if b > 0:
                    kbs = (key * jnp.exp(lastb - cb)).astype(BF16)
                    growth[b] = (jnp.exp(lastb), mm_tn(value, kbs))
            for b in reversed(range(count)):
                at = slice(b * BLK, (b + 1) * BLK)
                whole = mixed[b] + mm_nt(readers[b], backward.astype(BF16))
                if b > 0:
                    backward = growth[b][0] * backward + growth[b][1]
                scale = lax.rsqrt(jnp.mean(whole * whole, axis=-1, keepdims=True) + 1e-06)
                heads_ref[at, column + h * dv : column + (h + 1) * dv] = (
                    whole * scale * gain[...] * silu(g[at, vown].astype(F32))
                ).astype(BF16)
        base += heads * dk
        column += heads * dv
    split = pa.shape[0]
    width = out.shape[1]
    tile = min(512, width)
    for j in range(width // tile):
        cols = slice(j * tile, (j + 1) * tile)
        out[:, cols] = (
            mm(heads_ref[:, :split], pa[:, cols]) + mm(heads_ref[:, split:], pb[:, cols])
        ).astype(BF16)


def settle_kernel(
    n, part, stream, gain, settled, columns, inbox, mid, midbox, outbox, cs, cr, ys, yr, send2, recv2
):
    me = lax.axis_index("tp")
    own = part.shape[0] // n
    wide = part.shape[1] // n
    core = lax.rem(me, 2)
    line = me // 2
    lines = n // 2
    greet([{"tp": lax.rem(me + k, n)} for k in range(1, n)])

    def rows_of(i):
        return pl.ds(pl.multiple_of(i * own, own), own)

    def cols_of(i):
        return pl.ds(pl.multiple_of(i * wide, wide), wide)

    def line_at(j):
        return lax.rem(line + j, lines)

    def to_core(j):
        i = line_at(j) * 2 + 1 - core
        return remote(
            part.at[rows_of(i), :], inbox.at[j], cs.at[j], cr.at[j], {"tp": me + 1 - 2 * core}
        )

    def to_line(j):
        return remote(mid.at[j], midbox.at[j], ys.at[j], yr.at[j], {"tp": line_at(j) * 2 + core})

    for j in reversed(range(lines)):
        to_core(j).start()
    for j in reversed(range(lines)):
        to_core(j).wait_recv()
        mine = part[rows_of(line_at(j) * 2 + core), :].astype(F32) + inbox[j].astype(F32)
        if j > 0:
            mid[j] = mine.astype(BF16)
            to_line(j).start()
        else:
            total = mine
    for j in range(1, lines):
        to_line(j).wait_recv()
        total = total + midbox[j].astype(F32)
    total = total.astype(BF16).astype(F32)
    value = layer_norm(stream[rows_of(me), :].astype(F32) + total, gain[...])
    settled[...] = value
    outbox[...] = value.astype(BF16)
    second = []
    for k in range(1, n):
        peer = lax.rem(me + k, n)
        copy = remote(
            outbox.at[:, cols_of(peer)], columns.at[rows_of(me), :], send2.at[k], recv2.at[k], {"tp": peer}
        )
        copy.start()
        second.append(copy)
    columns[rows_of(me), :] = outbox[:, cols_of(me)]
    for k in range(1, n):
        source = lax.rem(me + n - k, n)
        second[k - 1].wait_send()
        remote(
            outbox.at[:, cols_of(source)], columns.at[rows_of(source), :], send2.at[k], recv2.at[k], {"tp": source}
        ).wait_recv()
    for j in range(lines):
        to_core(j).wait_send()
        if j > 0:
            to_line(j).wait_send()


def slots_of(routes, capacity, experts):
    top, rows = routes.shape
    levels = -(-max(16, experts) // 16) * 16
    level = lax.broadcasted_iota(jnp.int32, (levels, rows), 0)
    hots = [routes[i : i + 1] == level for i in range(top)]
    named = sum(jnp.where(h, 1.0, 0.0) for h in hots)
    ii = lax.broadcasted_iota(jnp.int32, (rows, rows), 0)
    jj = lax.broadcasted_iota(jnp.int32, (rows, rows), 1)
    before = mm(named.astype(BF16), jnp.where(ii < jj, 1.0, 0.0).astype(BF16))
    slots = []
    for i in range(top):
        rank = jnp.sum(jnp.where(hots[i], before, 0.0), axis=0, keepdims=True).astype(jnp.int32)
        slots.append(routes[i : i + 1] * capacity + rank)
    return slots


def experts_kernel(
    n, m, capacity, routes, affinity, columns, settled, gain, gate_hbm, up_hbm, down_hbm, out,
    wg, wu, wd, outgoing, x, part, inbox, mid, midbox, last, pieces, total, term, mixture,
    loads, ss, sr, ys, yr, cs, cr, fs, fr, rcs, rcr, rys, ryr, rss, rsr, send, recv,
):
    me = lax.axis_index("sp")
    my = lax.axis_index("tp")
    local = wg.shape[0]
    room = x.shape[1]
    experts = local * n
    top, rows = routes.shape
    wide = columns.shape[1]
    own = rows // m
    core = lax.rem(my, 2)
    line = my // 2
    lines = m // 2
    partner = my + 1 - 2 * core

    weights = [
        pltpu.make_async_copy(src, dst, loads.at[i])
        for i, (src, dst) in enumerate(((gate_hbm, wg), (up_hbm, wu), (down_hbm, wd)))
    ]
    for copy in weights:
        copy.start()

    greet(
        [{"sp": lax.rem(me + k, n)} for k in range(1, n)] + [{"tp": lax.rem(my + k, m)} for k in range(1, m)]
    )

    def cols_of(i):
        return pl.ds(pl.multiple_of(i * wide, wide), wide)

    def rows_of(i):
        return pl.ds(pl.multiple_of(i * own, own), own)

    def line_at(j):
        return lax.rem(line + j, lines)

    def line_source(j):
        return lax.rem(line + lines - j, lines)

    def peer(k):
        return across(me, k, n)

    def block(k, i):
        return x.at[k, :, cols_of(i)]

    def cross(k):
        return remote(outgoing.at[k], block(k, my), ss.at[k], sr.at[k], {"sp": peer(k)})

    def to_line(k, j, i):
        return remote(block(k, i), block(k, i), ys.at[k, j], yr.at[k, j], {"tp": line_at(j) * 2 + core})

    def to_core(k, i):
        return remote(block(k, i), block(k, i), cs.at[k], cr.at[k], {"tp": partner})

    def forward(k, j, i):
        return remote(block(k, i), block(k, i), fs.at[k, j], fr.at[k, j], {"tp": partner})

    def hand_on(k):
        if k > 0:
            cross(k).wait_recv()
        for j in range(1, lines):
            to_line(k, j, my).start()
        to_core(k, my).start()

    def pass_on(k):
        for j in range(1, lines):
            i = line_source(j) * 2 + core
            to_line(k, j, i).wait_recv()
            forward(k, j, i).start()

    def arrive(k):
        to_core(k, partner).wait_recv()
        for j in range(1, lines):
            forward(k, j, line_source(j) * 2 + 1 - core).wait_recv()

    def back_core(k, j):
        i = line_at(j) * 2 + 1 - core
        return remote(part.at[k, :, cols_of(i)], inbox.at[k, j], rcs.at[k, j], rcr.at[k, j], {"tp": partner})

    def back_line(k, j):
        return remote(
            mid.at[k, j], midbox.at[k, j], rys.at[k, j], ryr.at[k, j], {"tp": line_at(j) * 2 + core}
        )

    def back_cross(k):
        return remote(last.at[k], pieces.at[k], rss.at[k], rsr.at[k], {"sp": peer(k)})

    def back_start(k):
        for j in reversed(range(lines)):
            back_core(k, j).start()

    def back_first(k):
        for j in reversed(range(lines)):
            back_core(k, j).wait_recv()
            i = line_at(j) * 2 + core
            mine = part[k, :, cols_of(i)].astype(F32) + inbox[k, j].astype(F32)
            mid[k, j] = mine.astype(BF16)
            if j > 0:
                back_line(k, j).start()

    def back_second(k):
        value = mid[k, 0].astype(F32)
        for j in range(1, lines):
            back_line(k, j).wait_recv()
            value = value + midbox[k, j].astype(F32)
        if k > 0:
            last[k] = value.astype(BF16)
            back_cross(k).start()
        else:
            pieces[k] = value.astype(BF16)

    slots = slots_of(routes[...], capacity, experts)
    seat = lax.broadcasted_iota(jnp.int32, (room, rows), 0)
    for k in range(n):
        base = peer(k) * room
        hot = sum(jnp.where(seat == s - base, 1.0, 0.0) for s in slots).astype(BF16)
        picked = mm(hot, columns[...]).astype(BF16)
        if k == 0:
            x[0, :, cols_of(my)] = picked
            hand_on(0)
        else:
            outgoing[k] = picked
            cross(k).start()

    share = affinity[...] / jnp.sum(affinity[...], axis=0, keepdims=True)
    sheet = [s.astype(F32) for s in slots] + [share[i : i + 1] for i in range(top)]
    level = lax.broadcasted_iota(jnp.int32, (8, rows), 0)
    sheet = sum(jnp.where(level == i, r, 0.0) for i, r in enumerate(sheet)).T
    total[...] = jnp.zeros_like(total)

    def gather(k):
        if k > 0:
            back_cross(k).wait_recv()
        seats = lax.broadcasted_iota(jnp.int32, (rows, capacity), 1).astype(F32)
        value = total[...]
        for e in range(local):
            base = ((peer(k) * local + e) * capacity).astype(F32)
            rank = jnp.full((rows, 1), -1.0, F32)
            scale = jnp.zeros((rows, 1), F32)
            for i in range(top):
                at = sheet[:, i : i + 1] - base
                here = (at >= 0.0) & (at < capacity)
                rank = jnp.where(here, at, rank)
                scale = jnp.where(here, sheet[:, top + i : top + i + 1], scale)
            hot = jnp.where(seats == rank, 1.0, 0.0).astype(BF16)
            value = value + scale * mm(hot, pieces[k, e * capacity : (e + 1) * capacity, :])
        total[...] = value

    def multiply(first, count):
        for e in range(local):
            at = slice(e * capacity, (e + 1) * capacity)
            xe = [x[k, at, :] for k in range(first, first + count)]
            xe = xe[0] if count == 1 else jnp.concatenate(xe, axis=0)
            act = (silu(mm(xe, wg[e])) * mm(xe, wu[e])).astype(BF16)
            width = x.shape[2]
            tile = min(512, width)
            for c in range(width // tile):
                cols = slice(c * tile, (c + 1) * tile)
                value = mm(act, wd[e, :, cols]).astype(BF16)
                for k in range(count):
                    part[first + k, at, cols] = value[k * capacity : (k + 1) * capacity]

    group = 2 if n % 2 == 0 and capacity % 16 == 0 else 1
    ahead = group + 1
    for k in range(1, min(n, ahead + 1)):
        hand_on(k)
        pass_on(k - 1)
    if n <= ahead:
        pass_on(n - 1)
    groups = n // group
    for p in range(groups):
        mine = range(p * group, (p + 1) * group)
        for k in mine:
            arrive(k)
        if p == 0:
            for copy in weights:
                copy.wait()
        multiply(p * group, group)
        for k in mine:
            back_start(k)
        if p > 0:
            for k in range((p - 1) * group, p * group):
                back_second(k)
        for k in mine:
            if k + ahead < n:
                pass_on(k + ahead)
            if k + ahead + 1 < n:
                hand_on(k + ahead + 1)
            back_first(k)
        if p > 1:
            for k in range((p - 2) * group, (p - 1) * group):
                gather(k)
    for k in range((groups - 1) * group, n):
        back_second(k)
    for k in range(max(0, groups - 2) * group, n):
        gather(k)
    term[...] = total[...].astype(BF16)

    def swap(k, source, target):
        return remote(
            term.at[rows_of(source), :], mixture.at[:, cols_of(target)], send.at[k], recv.at[k], {"tp": source}
        )

    for k in range(1, m):
        swap(k, lax.rem(my + k, m), my).start()
    mixture[:, cols_of(my)] = term[rows_of(my), :]
    for k in range(n):
        if k > 0:
            cross(k).wait_send()
            back_cross(k).wait_send()
        to_core(k, my).wait_send()
        for j in range(1, lines):
            i = line_source(j) * 2 + core
            to_line(k, j, my).wait_send()
            forward(k, j, i).wait_send()
        for j in range(lines):
            back_core(k, j).wait_send()
            if j > 0:
                back_line(k, j).wait_send()
    for k in range(1, m):
        source = lax.rem(my + m - k, m)
        swap(k, source, source).wait_recv()
    for k in range(1, m):
        swap(k, lax.rem(my + k, m), my).wait_send()
    out[...] = layer_norm(settled[...] + mixture[...].astype(F32), gain[...]).astype(BF16)


def call(kernel, outs, scratch, count, collective_id=None):
    single = not isinstance(outs, list)
    return pl.pallas_call(
        kernel,
        out_shape=outs,
        in_specs=[VMEM] * count,
        out_specs=VMEM if single else [VMEM] * len(outs),
        scratch_shapes=scratch,
        compiler_params=params(collective_id),
    )


def body(
    query_one,
    key_one,
    value_one,
    gate_one,
    decay_one,
    query_two,
    key_two,
    value_two,
    gate_two,
    decay_two,
    head_gain,
    proj_one,
    proj_two,
    stream,
    gain_mix,
    gain_moe,
    routes,
    affinity,
    expert_gate,
    expert_up,
    expert_down,
):
    shape = jax.ShapeDtypeStruct
    rows = query_one.shape[0]
    n = lax.axis_size("sp")
    m = lax.axis_size("tp")
    width = stream.shape[1]
    own = rows // m
    wide = width // m
    dv = head_gain.shape[0]
    lanes = query_one.shape[1] + query_two.shape[1]
    values = value_one.shape[1] + value_two.shape[1]
    local_experts = expert_gate.shape[0]
    experts = local_experts * n
    top = routes.shape[1]
    capacity = 3 * rows * top // (2 * experts)
    room = local_experts * capacity

    half = dv // 2
    stack, cum = call(
        state_kernel, [shape((2, 2, half + 16, lanes), BF16), shape((2, rows, lanes), F32)], [], 6
    )(key_one, value_one, decay_one, key_two, value_two, decay_two)
    chunks = max(1, lanes // 256)
    states = call(
        functools.partial(states_exchange_kernel, n),
        shape((2, 2, half, lanes), BF16),
        [
            pltpu.VMEM((2, half + 16, lanes), BF16),
            pltpu.VMEM((2, half + 16, lanes), BF16),
            pltpu.VMEM((n // 2, half + 16, lanes), BF16),
            pltpu.VMEM((2, half, lanes), BF16),
            DMA((chunks,)), DMA((chunks,)), DMA((chunks, n // 2)), DMA((chunks, n // 2)),
            DMA((chunks,)), DMA((chunks,)),
        ],
        1,
        1,
    )(stack)
    part = call(mix_kernel, shape((rows, width), BF16), [pltpu.VMEM((rows, values), BF16)], 13)(
        states, cum, query_one, key_one, value_one, gate_one, query_two, key_two, value_two, gate_two,
        head_gain.reshape(1, -1), proj_one, proj_two,
    )
    settled, columns = call(
        functools.partial(settle_kernel, m),
        [shape((own, width), F32), shape((rows, wide), BF16)],
        [pltpu.VMEM((m // 2, own, width), BF16)] * 3
        + [pltpu.VMEM((own, width), BF16)]
        + [DMA((m // 2,))] * 4
        + [DMA((m,))] * 2,
        3,
        2,
    )(part, stream, gain_mix.reshape(1, -1))
    lines = m // 2
    tall = pltpu.VMEM((n, lines, room, wide), BF16)
    flat = pltpu.VMEM((n, room, wide), BF16)
    whole = pltpu.VMEM((n, room, width), BF16)
    hbm = pl.BlockSpec(memory_space=pl.ANY)
    return pl.pallas_call(
        functools.partial(experts_kernel, n, m, capacity),
        out_shape=shape((own, width), BF16),
        in_specs=[VMEM] * 5 + [hbm] * 3,
        out_specs=VMEM,
        scratch_shapes=[
            pltpu.VMEM(expert_gate.shape, BF16), pltpu.VMEM(expert_up.shape, BF16),
            pltpu.VMEM(expert_down.shape, BF16),
            flat, whole, whole, tall, tall, tall, flat, flat,
            pltpu.VMEM((rows, wide), F32), pltpu.VMEM((rows, wide), BF16), pltpu.VMEM((own, width), BF16),
            DMA((3,)), DMA((n,)), DMA((n,)), DMA((n, lines)), DMA((n, lines)), DMA((n,)), DMA((n,)),
            DMA((n, lines)), DMA((n, lines)), DMA((n, lines)), DMA((n, lines)), DMA((n, lines)), DMA((n, lines)),
            DMA((n,)), DMA((n,)), DMA((m,)), DMA((m,)),
        ],
        compiler_params=params(3),
    )(
        routes.T, affinity.T, columns, settled, gain_moe.reshape(1, -1), expert_gate, expert_up, expert_down
    )


def solution(mesh):
    return jax.shard_map(
        body,
        mesh=mesh,
        in_specs=(
            P("sp", "tp"),
            P("sp", "tp"),
            P("sp", "tp"),
            P("sp", "tp"),
            P(None, "sp", "tp"),
            P("sp", "tp"),
            P("sp", "tp"),
            P("sp", "tp"),
            P("sp", "tp"),
            P(None, "sp", "tp"),
            P(),
            P("tp", None),
            P("tp", None),
            P("sp", None),
            P(),
            P(),
            P("sp", None),
            P("sp", None),
            P("sp", None, "tp"),
            P("sp", None, "tp"),
            P("sp", "tp", None),
        ),
        out_specs=P(("sp", "tp"), None),
        check_vma=False,
    )
```

```python
import functools

import jax
import jax.numpy as jnp
from jax import lax
from jax.experimental import pallas as pl
from jax.experimental.pallas import tpu as pltpu
from jax.sharding import PartitionSpec as P

DK_A = 64
DK_B = 128
BLK = 64
SHARPNESS = 16.0
F32 = jnp.float32
BF16 = jnp.bfloat16
MESH = pl.DeviceIdType.MESH
VMEM = pl.BlockSpec(memory_space=pltpu.VMEM)
DMA = pltpu.SemaphoreType.DMA


def params(collective_id):
    return pltpu.CompilerParams(
        vmem_limit_bytes=60 * 2**20, collective_id=collective_id, has_side_effects=True
    )


def mm(a, b):
    return jnp.dot(a, b, preferred_element_type=F32)


def mm_nt(a, b):
    return lax.dot_general(a, b, (((1,), (1,)), ((), ())), preferred_element_type=F32)


def mm_tn(a, b):
    return lax.dot_general(a, b, (((0,), (0,)), ((), ())), preferred_element_type=F32)


def log_sigmoid(x):
    return jnp.minimum(x, 0.0) - jnp.log1p(jnp.exp(-jnp.abs(x)))


def silu(x):
    return x / (1.0 + jnp.exp(-x))


def layer_norm(values, gain):
    mean = jnp.mean(values, axis=-1, keepdims=True)
    spread = jnp.mean(jnp.square(values - mean), axis=-1, keepdims=True)
    return (values - mean) * lax.rsqrt(spread + 1e-05) * gain


def remote(src, dst, send, recv, peer):
    return pltpu.make_async_remote_copy(
        src_ref=src, dst_ref=dst, send_sem=send, recv_sem=recv, device_id=peer, device_id_type=MESH
    )


def across(me, k, n):
    place, bit = 0, 1
    while bit < n:
        digit = lax.rem(me // bit, 2)
        place = place + (1 - digit if k & bit else digit) * bit
        bit *= 2
    return place


def mixer(n, m, refs, scratch, sems, gain, gain_mix, columns, settled):
    qa, ka, va, ga, da, qb, kb, vb, gb, db, pa, pb, stream = refs
    stack, xbox, agg, zbox, outbox, states, fades, xfade, pfade, zfade, cum, mixed, readers, heads_ref = scratch[:14]
    part, inbox, mid, midbox, outbox_mix = scratch[14:]
    loads, xs, xr, xfs, xfr, zs, zr, zfs, zfr, bs, br, cs, cr, ys, yr, send2, recv2 = sems
    start, ready = loads
    me = lax.axis_index("sp")
    my = lax.axis_index("tp")
    rows = qa.shape[0]
    count = rows // BLK
    dv = gain.shape[1]
    half = dv // 2
    lanes = stack.shape[3]
    groups = ((qa, ka, va, ga, da, DK_A), (qb, kb, vb, gb, db, DK_B))
    side = lax.rem(me, 2)
    pair = me // 2
    pairs = n // 2
    partner = me + 1 - 2 * side
    chunk = 128 if all(g[1].shape[1] % 128 == 0 for g in groups) else lanes
    chunks = lanes // chunk

    def pair_at(j):
        return lax.rem(pair + j, pairs)

    def at(c):
        return pl.ds(c * chunk, chunk)

    def swap(c):
        return (
            remote(stack.at[1 - side, :, :, at(c)], xbox.at[:, :, at(c)], xs.at[c], xr.at[c], {"sp": partner}),
            remote(fades.at[:, :, at(c)], xfade.at[:, :, at(c)], xfs.at[c], xfr.at[c], {"sp": partner}),
        )

    def along(c, j):
        way = jnp.where(pair_at(j) < pair, 1, 0)
        peer = {"sp": pair_at(j) * 2 + side}
        return (
            remote(agg.at[way, :, at(c)], zbox.at[pair, :, at(c)], zs.at[c, j], zr.at[c, j], peer),
            remote(pfade.at[way, :, at(c)], zfade.at[pair, :, at(c)], zfs.at[c, j], zfr.at[c, j], peer),
        )

    def back(c, to):
        return remote(outbox.at[:, :, at(c)], states.at[:, to, :, at(c)], bs.at[c], br.at[c], {"sp": partner})

    def state(g, base):
        _, k, v, _, d, dk = groups[g]
        ii = lax.broadcasted_iota(jnp.int32, (rows, rows), 0)
        jj = lax.broadcasted_iota(jnp.int32, (rows, rows), 1)
        same = (ii // BLK) == (jj // BLK)
        wide = k.shape[1]
        heads = wide // dk
        keys = k[...].astype(F32)
        for way in range(2):
            fade = log_sigmoid(d[way]) / SHARPNESS
            high = fade.astype(BF16)
            low = (fade - high.astype(F32)).astype(BF16)
            tri = jnp.where(same & (ii >= jj if way == 0 else ii <= jj), 1.0, 0.0).astype(BF16)
            total = mm(tri, high) + mm(tri, low)
            cum[way, :, base : base + wide] = total
            tail = jnp.zeros((1, wide), F32)
            weighted = [None] * count
            for b in reversed(range(count)) if way == 0 else range(count):
                piece = total[b * BLK : (b + 1) * BLK]
                final = piece[BLK - 1 : BLK] if way == 0 else piece[0:1]
                weighted[b] = (keys[b * BLK : (b + 1) * BLK] * jnp.exp(final - piece + tail)).astype(BF16)
                tail = tail + final
            weighted = jnp.concatenate(weighted, axis=0)
            out = [
                mm_tn(v[:, h * dv : (h + 1) * dv], weighted[:, h * dk : (h + 1) * dk]).astype(BF16)
                for h in range(heads)
            ]
            out = out[0] if heads == 1 else jnp.concatenate(out, axis=1)
            for i in range(2):
                stack[i, way, :, base : base + wide] = out[i * half : (i + 1) * half]
            fades[way, :, base : base + wide] = tail

    def local(g, h, base, column):
        q, k, v, _, _, dk = groups[g]
        ii = lax.broadcasted_iota(jnp.int32, (BLK, BLK), 0)
        jj = lax.broadcasted_iota(jnp.int32, (BLK, BLK), 1)
        span = slice(base + h * dk, base + (h + 1) * dk)
        own = slice(h * dk, (h + 1) * dk)
        vown = slice(h * dv, (h + 1) * dv)
        place = slice(column + h * dv, column + (h + 1) * dv)
        result = [None] * count
        reads = [None] * count
        growth = [None] * count
        forward = None
        passed = jnp.zeros((1, dk), F32)
        for b in range(count):
            bat = slice(b * BLK, (b + 1) * BLK)
            query = q[bat, own].astype(F32) * dk ** (-0.5)
            key = k[bat, own].astype(F32)
            value = v[bat, vown]
            cf = cum[0, bat, span]
            cb = cum[1, bat, span]
            grown = query * jnp.exp(cf)
            qf = grown.astype(BF16)
            kf = (key * jnp.exp(-cf)).astype(BF16)
            reads[b] = query * jnp.exp(cb)
            qr = reads[b].astype(BF16)
            kr = (key * jnp.exp(-cb)).astype(BF16)
            scores = jnp.where(ii >= jj, mm_nt(qf, kf), 0.0) + jnp.where(ii <= jj, mm_nt(qr, kr), 0.0)
            inner = mm(scores.astype(BF16), value)
            lastf = cf[BLK - 1 : BLK]
            if b > 0:
                inner = inner + mm_nt(qf, forward.astype(BF16))
            readers[0, bat, span] = qf if b == 0 else (grown * jnp.exp(passed)).astype(BF16)
            passed = passed + lastf
            if b < count - 1:
                kfs = (key * jnp.exp(lastf - cf)).astype(BF16)
                added = mm_tn(value, kfs)
                forward = added if b == 0 else jnp.exp(lastf) * forward + added
            result[b] = inner
            lastb = cb[0:1]
            growth[b] = (lastb, mm_tn(value, (key * jnp.exp(lastb - cb)).astype(BF16)) if b > 0 else None)
        backward = None
        passed = jnp.zeros((1, dk), F32)
        for b in reversed(range(count)):
            bat = slice(b * BLK, (b + 1) * BLK)
            whole = result[b]
            if b < count - 1:
                whole = whole + mm_nt(reads[b].astype(BF16), backward.astype(BF16))
            mixed[bat, place] = whole
            readers[1, bat, span] = (reads[b] * jnp.exp(passed)).astype(BF16)
            passed = passed + growth[b][0]
            if b > 0:
                added = growth[b][1]
                backward = added if b == count - 1 else jnp.exp(growth[b][0]) * backward + added

    def settle_head(g, h, base, column):
        _, _, _, gate, _, dk = groups[g]
        span = slice(base + h * dk, base + (h + 1) * dk)
        vown = slice(h * dv, (h + 1) * dv)
        place = slice(column + h * dv, column + (h + 1) * dv)
        whole = mixed[:, place]
        for way in range(2):
            whole = whole + mm_nt(
                readers[way, :, span], jnp.concatenate([states[way, i, :, span] for i in range(2)], axis=0)
            )
        scale = lax.rsqrt(jnp.mean(whole * whole, axis=-1, keepdims=True) + 1e-06)
        heads_ref[:, place] = (whole * scale * gain[...] * silu(gate[:, vown].astype(F32))).astype(BF16)

    def both(c, way):
        own = stack[side, way, :, at(c)].astype(F32)
        other = xbox[way, :, at(c)].astype(F32)
        own_fade = fades[way, :, at(c)]
        other_fade = xfade[way, :, at(c)]
        low = side == 0
        return (
            jnp.where(low, own, other), jnp.where(low, own_fade, other_fade),
            jnp.where(low, other, own), jnp.where(low, other_fade, own_fade),
        )

    def first(c):
        for copy in swap(c):
            copy.wait_recv()
        s0, t0, s1, t1 = both(c, 0)
        agg[0, :, at(c)] = (jnp.exp(t1) * s0 + s1).astype(BF16)
        pfade[0, :, at(c)] = t0 + t1
        s0, t0, s1, t1 = both(c, 1)
        agg[1, :, at(c)] = (jnp.exp(t0) * s1 + s0).astype(BF16)
        pfade[1, :, at(c)] = t0 + t1
        for j in range(1, pairs):
            for copy in along(c, j):
                copy.start()

    def second(c):
        for j in range(1, pairs):
            for copy in along(c, j):
                copy.wait_recv()
        ahead = jnp.zeros((half, chunk), F32)
        behind = jnp.zeros((half, chunk), F32)
        for s in range(pairs):
            ahead = jnp.where(
                s < pair, jnp.exp(zfade[s, :, at(c)]) * ahead + zbox[s, :, at(c)].astype(F32), ahead
            )
        for s in reversed(range(pairs)):
            behind = jnp.where(
                s > pair, jnp.exp(zfade[s, :, at(c)]) * behind + zbox[s, :, at(c)].astype(F32), behind
            )
        low = side == 0
        s0, t0, _, _ = both(c, 0)
        next_ahead = jnp.exp(t0) * ahead + s0
        _, _, s1, t1 = both(c, 1)
        next_behind = jnp.exp(t1) * behind + s1
        outbox[0, :, at(c)] = jnp.where(low, next_ahead, ahead).astype(BF16)
        outbox[1, :, at(c)] = jnp.where(low, behind, next_behind).astype(BF16)
        back(c, side).start()
        states[0, side, :, at(c)] = jnp.where(low, ahead, next_ahead).astype(BF16)
        states[1, side, :, at(c)] = jnp.where(low, next_behind, behind).astype(BF16)

    zbox[pair] = jnp.zeros_like(zbox[pair])
    zfade[pair] = jnp.zeros_like(zfade[pair])
    heads = []
    base = 0
    column = 0
    for g, (_, k, v, _, _, dk) in enumerate(groups):
        ready(g)
        state(g, base)
        for h in range(k.shape[1] // dk):
            heads.append((g, h, base, column))
        base += k.shape[1]
        column += v.shape[1]
    start()
    for c in range(chunks):
        for copy in swap(c):
            copy.start()
    ready(2)
    events = [functools.partial(first, c) for c in range(chunks)] + [
        functools.partial(second, c) for c in range(chunks)
    ]
    early = min(2, len(heads))
    for head in heads[:early]:
        local(*head)
    rest = heads[early:]
    span = max(1, len(events) - 2)
    done = 0
    for i, event in enumerate(events):
        event()
        while done < len(rest) and done * span < (i + 1) * len(rest):
            local(*rest[done])
            done += 1
    for head in rest[done:]:
        local(*head)
    ended = 0
    for c in range(chunks):
        back(c, 1 - side).wait_recv()
        while ended < len(heads):
            g, h, base, _ = heads[ended]
            if base + (h + 1) * groups[g][5] > (c + 1) * chunk:
                break
            settle_head(*heads[ended])
            ended += 1

    ready(3)
    own = rows // m
    wide = columns.shape[1]
    width = part.shape[1]
    tile = min(512, width)
    tiles = width // tile
    core = lax.rem(my, 2)
    line = my // 2
    lines = m // 2
    split = pa.shape[0]

    def rows_of(i):
        return pl.ds(pl.multiple_of(i * own, own), own)

    def cols_of(i):
        return pl.ds(pl.multiple_of(i * wide, wide), wide)

    def line_at(j):
        return lax.rem(line + j, lines)

    def to_core(j, t):
        i = line_at(j) * 2 + 1 - core
        cut = pl.ds(t * tile, tile)
        return remote(
            part.at[rows_of(i), cut], inbox.at[j, :, cut], cs.at[j, t], cr.at[j, t], {"tp": my + 1 - 2 * core}
        )

    def to_line(j, t):
        cut = pl.ds(t * tile, tile)
        return remote(
            mid.at[j, :, cut], midbox.at[j, :, cut], ys.at[j, t], yr.at[j, t], {"tp": line_at(j) * 2 + core}
        )

    def project(t):
        cut = slice(t * tile, (t + 1) * tile)
        part[:, cut] = (mm(heads_ref[:, :split], pa[:, cut]) + mm(heads_ref[:, split:], pb[:, cut])).astype(BF16)
        for j in reversed(range(lines)):
            to_core(j, t).start()

    def add_core(t):
        cut = slice(t * tile, (t + 1) * tile)
        for j in reversed(range(lines)):
            to_core(j, t).wait_recv()
            mine = part[rows_of(line_at(j) * 2 + core), cut].astype(F32) + inbox[j, :, cut].astype(F32)
            if j > 0:
                mid[j, :, cut] = mine.astype(BF16)
                to_line(j, t).start()
            else:
                settled[:, cut] = mine

    def add_line(t):
        cut = slice(t * tile, (t + 1) * tile)
        value = settled[:, cut]
        for j in range(1, lines):
            to_line(j, t).wait_recv()
            value = value + midbox[j, :, cut].astype(F32)
        settled[:, cut] = stream[:, cut].astype(F32) + value.astype(BF16).astype(F32)

    for t in range(tiles):
        project(t)
        if t > 1:
            add_core(t - 2)
    for t in range(max(0, tiles - 2), tiles):
        add_core(t)
    for t in range(tiles):
        add_line(t)
    value = layer_norm(settled[...], gain_mix[...])
    settled[...] = value
    outbox_mix[...] = value.astype(BF16)

    def second_copy(k, source, target, peer):
        return remote(
            outbox_mix.at[:, cols_of(target)], columns.at[rows_of(source), :], send2.at[k], recv2.at[k], {"tp": peer}
        )

    order = [k for k in range(1, m) if k % 2 == 0] + [k for k in range(1, m) if k % 2 == 1]
    for k in order:
        peer = lax.rem(my + k, m)
        second_copy(k, my, peer, peer).start()
    columns[rows_of(my), :] = outbox_mix[:, cols_of(my)]
    for c in range(chunks):
        for copy in swap(c):
            copy.wait_send()
        for j in range(1, pairs):
            for copy in along(c, j):
                copy.wait_send()
        back(c, side).wait_send()
    for t in range(tiles):
        for j in range(lines):
            to_core(j, t).wait_send()
            if j > 0:
                to_line(j, t).wait_send()
    for k in range(1, m):
        source = lax.rem(my + m - k, m)
        second_copy(k, source, source, source).wait_recv()
    for k in range(1, m):
        peer = lax.rem(my + k, m)
        second_copy(k, my, peer, peer).wait_send()


def slots_of(routes, capacity, experts):
    top, rows = routes.shape
    levels = -(-max(16, experts) // 16) * 16
    level = lax.broadcasted_iota(jnp.int32, (levels, rows), 0)
    hots = [routes[i : i + 1] == level for i in range(top)]
    named = sum(jnp.where(h, 1.0, 0.0) for h in hots)
    ii = lax.broadcasted_iota(jnp.int32, (rows, rows), 0)
    jj = lax.broadcasted_iota(jnp.int32, (rows, rows), 1)
    before = mm(named.astype(BF16), jnp.where(ii < jj, 1.0, 0.0).astype(BF16))
    slots = []
    for i in range(top):
        rank = jnp.sum(jnp.where(hots[i], before, 0.0), axis=0, keepdims=True).astype(jnp.int32)
        slots.append(routes[i : i + 1] * capacity + rank)
    return slots


def experts_phase(n, m, capacity, routes, affinity, columns, settled, gain, weights, out, scratch, sems):
    wg, wu, wd, outgoing, x, part, inbox, mid, midbox, last, pieces, total, term, mixture = scratch
    ss, sr, ys, yr, cs, cr, fs, fr, rcs, rcr, rys, ryr, rss, rsr, send, recv = sems
    me = lax.axis_index("sp")
    my = lax.axis_index("tp")
    local = wg.shape[0]
    room = x.shape[1]
    experts = local * n
    top, rows = routes.shape
    wide = columns.shape[1]
    own = rows // m
    core = lax.rem(my, 2)
    line = my // 2
    lines = m // 2
    partner = my + 1 - 2 * core

    def cols_of(i):
        return pl.ds(pl.multiple_of(i * wide, wide), wide)

    def rows_of(i):
        return pl.ds(pl.multiple_of(i * own, own), own)

    def line_at(j):
        return lax.rem(line + j, lines)

    def line_source(j):
        return lax.rem(line + lines - j, lines)

    def peer(k):
        return across(me, k, n)

    def block(k, i):
        return x.at[k, :, cols_of(i)]

    def cross(k):
        return remote(outgoing.at[k], block(k, my), ss.at[k], sr.at[k], {"sp": peer(k)})

    def to_line(k, j, i):
        return remote(block(k, i), block(k, i), ys.at[k, j], yr.at[k, j], {"tp": line_at(j) * 2 + core})

    def to_core(k, i):
        return remote(block(k, i), block(k, i), cs.at[k], cr.at[k], {"tp": partner})

    def forward(k, j, i):
        return remote(block(k, i), block(k, i), fs.at[k, j], fr.at[k, j], {"tp": partner})

    def hand_on(k):
        if k > 0:
            cross(k).wait_recv()
        for j in range(1, lines):
            to_line(k, j, my).start()
        to_core(k, my).start()

    def pass_on(k):
        for j in range(1, lines):
            i = line_source(j) * 2 + core
            to_line(k, j, i).wait_recv()
            forward(k, j, i).start()

    def arrive(k):
        to_core(k, partner).wait_recv()
        for j in range(1, lines):
            forward(k, j, line_source(j) * 2 + 1 - core).wait_recv()

    def back_core(k, j):
        i = line_at(j) * 2 + 1 - core
        return remote(part.at[k, :, cols_of(i)], inbox.at[k, j], rcs.at[k, j], rcr.at[k, j], {"tp": partner})

    def back_line(k, j):
        return remote(
            mid.at[k, j], midbox.at[k, j], rys.at[k, j], ryr.at[k, j], {"tp": line_at(j) * 2 + core}
        )

    def back_cross(k):
        return remote(last.at[k], pieces.at[k], rss.at[k], rsr.at[k], {"sp": peer(k)})

    def back_start(k):
        for j in reversed(range(lines)):
            back_core(k, j).start()

    def back_first(k):
        for j in reversed(range(lines)):
            back_core(k, j).wait_recv()
            i = line_at(j) * 2 + core
            mine = part[k, :, cols_of(i)].astype(F32) + inbox[k, j].astype(F32)
            mid[k, j] = mine.astype(BF16)
            if j > 0:
                back_line(k, j).start()

    def back_second(k):
        value = mid[k, 0].astype(F32)
        for j in range(1, lines):
            back_line(k, j).wait_recv()
            value = value + midbox[k, j].astype(F32)
        if k > 0:
            last[k] = value.astype(BF16)
            back_cross(k).start()
        else:
            pieces[k] = value.astype(BF16)

    slots = slots_of(routes[...], capacity, experts)
    seat = lax.broadcasted_iota(jnp.int32, (room, rows), 0)
    far = list(range(n // 2, n - n // 4))
    near = [k for k in range(1, n) if k not in far]
    order = [0] + near[:1]
    for i in range(1, n):
        order += far[i - 1 : i] + near[i : i + 1]
    for k in order:
        base = peer(k) * room
        hot = sum(jnp.where(seat == s - base, 1.0, 0.0) for s in slots).astype(BF16)
        picked = mm(hot, columns[...]).astype(BF16)
        if k == 0:
            x[0, :, cols_of(my)] = picked
            hand_on(0)
        else:
            outgoing[k] = picked
            cross(k).start()

    share = affinity[...] / jnp.sum(affinity[...], axis=0, keepdims=True)
    sheet = [s.astype(F32) for s in slots] + [share[i : i + 1] for i in range(top)]
    level = lax.broadcasted_iota(jnp.int32, (8, rows), 0)
    sheet = sum(jnp.where(level == i, r, 0.0) for i, r in enumerate(sheet)).T
    total[...] = jnp.zeros_like(total)

    def gather(k):
        if k > 0:
            back_cross(k).wait_recv()
        seats = lax.broadcasted_iota(jnp.int32, (rows, capacity), 1).astype(F32)
        value = total[...]
        for e in range(local):
            base = ((peer(k) * local + e) * capacity).astype(F32)
            rank = jnp.full((rows, 1), -1.0, F32)
            scale = jnp.zeros((rows, 1), F32)
            for i in range(top):
                at = sheet[:, i : i + 1] - base
                here = (at >= 0.0) & (at < capacity)
                rank = jnp.where(here, at, rank)
                scale = jnp.where(here, sheet[:, top + i : top + i + 1], scale)
            hot = jnp.where(seats == rank, 1.0, 0.0).astype(BF16)
            value = value + scale * mm(hot, pieces[k, e * capacity : (e + 1) * capacity, :])
        total[...] = value

    def multiply(ks):
        for e in range(local):
            at = slice(e * capacity, (e + 1) * capacity)
            xe = [x[k, at, :] for k in ks]
            xe = xe[0] if len(xe) == 1 else jnp.concatenate(xe, axis=0)
            act = (silu(mm(xe, wg[e])) * mm(xe, wu[e])).astype(BF16)
            width = x.shape[2]
            tile = min(512, width)
            for c in range(width // tile):
                cols = slice(c * tile, (c + 1) * tile)
                value = mm(act, wd[e, :, cols]).astype(BF16)
                for i, k in enumerate(ks):
                    part[k, at, cols] = value[i * capacity : (i + 1) * capacity]

    group = 2 if n % 2 == 0 and capacity % 16 == 0 else 1
    handed = [0]
    passed = [-1]

    def hand_to(i):
        while handed[0] < min(i, n - 1):
            handed[0] += 1
            hand_on(order[handed[0]])

    def pass_to(i):
        while passed[0] < min(i, n - 1):
            hand_to(passed[0] + 1)
            passed[0] += 1
            pass_on(order[passed[0]])

    line_up = order[1:] + order[:1]
    sets = [line_up[i : i + group] for i in range(0, n, group)]
    hand_to(1)
    pass_to(0)
    hand_to(2)
    pass_to(1)
    hand_to(4)
    pass_to(2)
    hand_to(5)
    for p, ks in enumerate(sets):
        pass_to(group * (p + 1))
        for k in ks:
            arrive(k)
        if p == 0:
            for copy in weights:
                copy.wait()
        multiply(ks)
        for k in ks:
            back_start(k)
        pass_to(group * (p + 1) + 1)
        hand_to(group * (p + 1) + 4)
        if p > 1:
            for k in sets[p - 2]:
                back_second(k)
        for k in ks:
            back_first(k)
        hand_to(group * (p + 1) + 5)
        pass_to(group * (p + 2))
        if p > 2:
            for k in sets[p - 3]:
                gather(k)
    late = max(0, len(sets) - 2)
    for k in sets[late]:
        back_second(k)
    for p in range(max(0, len(sets) - 3), late):
        for k in sets[p]:
            gather(k)
    for p in range(late + 1, len(sets)):
        for k in sets[p]:
            back_second(k)
    for k in sets[late] + [k for ks in sets[late + 1 :] for k in reversed(ks)]:
        gather(k)
    term[...] = total[...].astype(BF16)

    def swap(k, source, target):
        return remote(
            term.at[rows_of(source), :], mixture.at[:, cols_of(target)], send.at[k], recv.at[k], {"tp": source}
        )

    for k in range(1, m):
        swap(k, lax.rem(my + k, m), my).start()
    mixture[:, cols_of(my)] = term[rows_of(my), :]
    for k in range(n):
        if k > 0:
            cross(k).wait_send()
            back_cross(k).wait_send()
        to_core(k, my).wait_send()
        for j in range(1, lines):
            i = line_source(j) * 2 + core
            to_line(k, j, my).wait_send()
            forward(k, j, i).wait_send()
        for j in range(lines):
            back_core(k, j).wait_send()
            if j > 0:
                back_line(k, j).wait_send()
    for k in range(1, m):
        source = lax.rem(my + m - k, m)
        swap(k, source, source).wait_recv()
    for k in range(1, m):
        swap(k, lax.rem(my + k, m), my).wait_send()
    out[...] = layer_norm(settled[...] + mixture[...].astype(F32), gain[...]).astype(BF16)


def layer_kernel(n, m, capacity, *refs):
    routes, affinity, gain, gain_mix, gain_moe = refs[:5]
    hbm = refs[5:21]
    out = refs[21]
    held = refs[22:38]
    rest = refs[38:]
    columns, settled = rest[:2]
    mix_scratch = rest[2:21]
    moe_scratch = rest[21:32]
    arrived = rest[32]
    mix_sems = rest[33:49]
    moe_sems = rest[49:65]
    my = lax.axis_index("tp")
    me = lax.axis_index("sp")
    own = settled.shape[0]
    names = (
        "qa", "ka", "va", "ga", "da", "qb", "kb", "vb", "gb", "db", "pa", "pb", "stream", "wg", "wu", "wd",
    )
    place = {name: i for i, name in enumerate(names)}

    def load(name):
        i = place[name]
        src = hbm[i]
        if name == "stream":
            src = src.at[pl.ds(pl.multiple_of(my * own, own), own), :]
        return pltpu.make_async_copy(src, held[i], arrived.at[i])

    stages = [["da", "ka", "va"], ["db", "kb", "vb"], ["qa", "qb"], ["ga", "gb", "pa", "pb", "stream"]]
    for stage in stages:
        for name in stage:
            load(name).start()
    barrier = pltpu.get_barrier_semaphore()
    peers = [{"sp": lax.rem(me + k, n)} for k in range(1, n)] + [{"tp": lax.rem(my + k, m)} for k in range(1, m)]
    for peer in peers:
        pl.semaphore_signal(barrier, inc=1, device_id=peer, device_id_type=MESH)

    def start():
        pl.semaphore_wait(barrier, len(peers))
        for name in ("wg", "wu", "wd"):
            load(name).start()

    def ready(stage):
        for name in stages[stage]:
            load(name).wait()
        if stage == 2:
            for name in ("ga", "gb"):
                load(name).wait()
            stages[3] = [name for name in stages[3] if name not in ("ga", "gb")]

    mixer(n, m, held[:13], mix_scratch, ((start, ready),) + mix_sems, gain, gain_mix, columns, settled)
    experts_phase(
        n, m, capacity, routes, affinity, columns, settled, gain_moe, [load(w) for w in ("wg", "wu", "wd")],
        out, held[13:] + moe_scratch, moe_sems,
    )


def body(
    query_one,
    key_one,
    value_one,
    gate_one,
    decay_one,
    query_two,
    key_two,
    value_two,
    gate_two,
    decay_two,
    head_gain,
    proj_one,
    proj_two,
    stream,
    gain_mix,
    gain_moe,
    routes,
    affinity,
    expert_gate,
    expert_up,
    expert_down,
):
    shape = jax.ShapeDtypeStruct
    rows = query_one.shape[0]
    n = lax.axis_size("sp")
    m = lax.axis_size("tp")
    width = stream.shape[1]
    own = rows // m
    wide = width // m
    dv = head_gain.shape[0]
    lanes = query_one.shape[1] + query_two.shape[1]
    values = value_one.shape[1] + value_two.shape[1]
    local_experts = expert_gate.shape[0]
    experts = local_experts * n
    top = routes.shape[1]
    capacity = 3 * rows * top // (2 * experts)
    room = local_experts * capacity

    half = dv // 2
    pairs = n // 2
    lines = m // 2
    chunk = 128 if query_one.shape[1] % 128 == 0 and query_two.shape[1] % 128 == 0 else lanes
    chunks = lanes // chunk
    tiles = max(1, width // 512)
    vmem = pltpu.VMEM
    tall = vmem((n, lines, room, wide), BF16)
    flat = vmem((n, room, wide), BF16)
    whole = vmem((n, room, width), BF16)
    hbm = pl.BlockSpec(memory_space=pl.ANY)
    arrays = [
        query_one, key_one, value_one, gate_one, decay_one, query_two, key_two, value_two, gate_two, decay_two,
        proj_one, proj_two, stream, expert_gate, expert_up, expert_down,
    ]
    held = [vmem((own, width) if a is stream else a.shape, a.dtype) for a in arrays]
    mix_scratch = [
        vmem((2, 2, half, lanes), BF16), vmem((2, half, lanes), BF16), vmem((2, half, lanes), BF16),
        vmem((pairs, half, lanes), BF16), vmem((2, half, lanes), BF16), vmem((2, 2, half, lanes), BF16),
        vmem((2, 1, lanes), F32), vmem((2, 1, lanes), F32), vmem((2, 1, lanes), F32), vmem((pairs, 1, lanes), F32),
        vmem((2, rows, lanes), F32), vmem((rows, values), F32), vmem((2, rows, lanes), BF16),
        vmem((rows, values), BF16),
        vmem((rows, width), BF16), vmem((lines, own, width), BF16), vmem((lines, own, width), BF16),
        vmem((lines, own, width), BF16), vmem((own, width), BF16),
    ]
    moe_scratch = [
        flat, whole, whole, tall, tall, tall, flat, flat,
        vmem((rows, wide), F32), vmem((rows, wide), BF16), vmem((own, width), BF16),
    ]
    mix_sems = [
        DMA((chunks,)), DMA((chunks,)), DMA((chunks,)), DMA((chunks,)),
        DMA((chunks, pairs)), DMA((chunks, pairs)), DMA((chunks, pairs)), DMA((chunks, pairs)),
        DMA((chunks,)), DMA((chunks,)),
        DMA((lines, tiles)), DMA((lines, tiles)), DMA((lines, tiles)), DMA((lines, tiles)),
        DMA((m,)), DMA((m,)),
    ]
    moe_sems = [
        DMA((n,)), DMA((n,)), DMA((n, lines)), DMA((n, lines)), DMA((n,)), DMA((n,)),
        DMA((n, lines)), DMA((n, lines)), DMA((n, lines)), DMA((n, lines)), DMA((n, lines)), DMA((n, lines)),
        DMA((n,)), DMA((n,)), DMA((m,)), DMA((m,)),
    ]
    return pl.pallas_call(
        functools.partial(layer_kernel, n, m, capacity),
        out_shape=shape((own, width), BF16),
        in_specs=[VMEM] * 5 + [hbm] * len(arrays),
        out_specs=VMEM,
        scratch_shapes=held
        + [vmem((rows, wide), BF16), vmem((own, width), F32)]
        + mix_scratch + moe_scratch + [DMA((len(arrays),))] + mix_sems + moe_sems,
        compiler_params=params(1),
    )(
        routes.T, affinity.T, head_gain.reshape(1, -1), gain_mix.reshape(1, -1), gain_moe.reshape(1, -1), *arrays
    )


def solution(mesh):
    return jax.shard_map(
        body,
        mesh=mesh,
        in_specs=(
            P("sp", "tp"),
            P("sp", "tp"),
            P("sp", "tp"),
            P("sp", "tp"),
            P(None, "sp", "tp"),
            P("sp", "tp"),
            P("sp", "tp"),
            P("sp", "tp"),
            P("sp", "tp"),
            P(None, "sp", "tp"),
            P(),
            P("tp", None),
            P("tp", None),
            P("sp", None),
            P(),
            P(),
            P("sp", None),
            P("sp", None),
            P("sp", None, "tp"),
            P("sp", None, "tp"),
            P("sp", "tp", None),
        ),
        out_specs=P(("sp", "tp"), None),
        check_vma=False,
    )
```
